32 devices in a mesh: sp: 8 (over z, y), tp: 4 (over x, core).
Axes of the slice: x: 2, y: 2, z: 4, core: 2. Of those that a mesh axis runs over, the one named last changes fastest.
Arguments:
- tokens: bfloat16 [3072, 2048], P(('sp', 'tp')), may hold values from -8 to 8, as said below
- query_weight: bfloat16 [2048, 1024], P(None, 'tp'), as said below
- key_weight: bfloat16 [2048, 256], P(None, 'tp'), as said below
- value_weight: bfloat16 [2048, 256], P(None, 'tp'), may hold values from -0.125 to 0.125
- out_weight: bfloat16 [1024, 2048], P('tp'), may hold values from -0.75 to 0.75
- query_gain: bfloat16 [16, 64], P('tp'), may hold values from 0.5 to 6.5
- key_gain: bfloat16 [4, 64], P('tp'), may hold values from 0.5 to 6.5
Outputs:
- mixed: bfloat16 [3072, 2048], P(('sp', 'tp'))
- log_sums: float32 [16, 3072], P('tp', 'sp')
The draws below stay inside these ranges and needn't reach their ends.
Inputs may be any that keep to these rules, and one draw needn't show every extreme that they name: Each block of 384 consecutive tokens has a mean vector of its own. `query_weight`: entries are those of a weight over 2048 inputs, of magnitude at most 6 / sqrt(2048). `key_weight`: entries are those of a weight over 2048 inputs, of magnitude at most 6 / sqrt(2048).
All inputs are finite; a program needn't handle non-finite values.
Results may differ from the reference program's by a relative error of at most 0.028.
Values may be sent and summed in bfloat16 or wider, within the bound.
A program may use at most 64 MiB of HBM per device.

```python
import math
import jax
import jax.numpy as jnp
from jax import lax

D = 2048
HEADS = 16
KV_HEADS = 4
HD = 64
GRID_W = 64
TOK_DEV = 384
TOKENS = 3072
N_TP = 4


def shared_query(key):
    base = jnp.clip(jax.random.normal(jax.random.fold_in(key, 11), (D, HEADS * HD), jnp.float32), -6.0, 6.0)
    base = base * D ** (-0.5)
    return base


def draw_tokens(key, part):
    offsets = jax.random.normal(jax.random.fold_in(key, 21), (TOKENS // TOK_DEV, D), jnp.float32)
    offsets = jnp.repeat(offsets, TOK_DEV, axis=0)
    noise = jax.random.normal(jax.random.fold_in(key, 22), (TOKENS, D), jnp.float32)
    return jnp.clip(noise + offsets, -8.0, 8.0).astype(jnp.bfloat16)


def draw_query_weight(key, part):
    return shared_query(key).astype(jnp.bfloat16)


def draw_key_weight(key, part):
    base = jnp.clip(jax.random.normal(jax.random.fold_in(key, 12), (D, KV_HEADS * HD), jnp.float32), -6.0, 6.0)
    return (base * D ** (-0.5)).astype(jnp.bfloat16)


def draw_query_gain(key, part):
    usual = jax.random.uniform(jax.random.fold_in(key, 31), (HEADS, HD), jnp.float32, 0.5, 1.5)
    return usual.astype(jnp.bfloat16)


def draw_key_gain(key, part):
    return jax.random.uniform(jax.random.fold_in(key, 41), (KV_HEADS, HD), jnp.float32, 0.5, 1.5).astype(jnp.bfloat16)


def level_of(key, shape, shards, low, largest):
    loudness = 1.0
    for dim, blocks in shards:
        draws = jax.random.uniform(jax.random.fold_in(jax.random.fold_in(key, 6), dim), (blocks,), jnp.float32, low / len(shards), largest / len(shards))
        loudness = loudness * jnp.repeat(jnp.exp(draws), shape[dim] // blocks).reshape((-1,) + (1,) * (len(shape) - 1 - dim))
    return loudness


def bell_draw(stream_key, dims, scale, reach, shards=(), held_as=jnp.bfloat16):
    loudness = level_of(stream_key, dims, shards, -0.22, 0.18) if shards else 1.0
    drawn = jax.random.normal(stream_key, dims, jnp.float32) * scale * loudness
    return jnp.minimum(jnp.maximum(drawn, -reach), reach).astype(held_as)


def setup_inputs(seed: int = 0) -> dict:
    key_of = jax.random.split(jax.random.key(seed), 8)
    return {
        "tokens": draw_tokens(jax.random.fold_in(key_of[7], 71), 0),
        "query_weight": draw_query_weight(jax.random.fold_in(key_of[7], 71), 0),
        "key_weight": draw_key_weight(jax.random.fold_in(key_of[7], 71), 0),
        "value_weight": bell_draw(key_of[3], (D, KV_HEADS * HD), D ** -0.5, 0.125, ((1, 4),)),
        "out_weight": bell_draw(key_of[4], (HEADS * HD, D), (HEADS * HD // 16) ** -0.5, 0.75, ((0, 4),)),
        "query_gain": draw_query_gain(jax.random.fold_in(key_of[7], 71), 0),
        "key_gain": draw_key_gain(jax.random.fold_in(key_of[7], 71), 0),
    }


def angle_tables(count):
    quarter = HD // 4
    place = jnp.arange(count, dtype=jnp.int32)
    grid_row = (place // GRID_W).astype(jnp.float32)
    grid_col = (place % GRID_W).astype(jnp.float32)
    freq = 10000.0 ** (-jnp.arange(quarter, dtype=jnp.float32).astype(jnp.float32) / quarter)
    row_angle = grid_row[:, None] * freq[None, :]
    col_angle = grid_col[:, None] * freq[None, :]
    return (jnp.cos(row_angle), jnp.sin(row_angle), jnp.cos(col_angle), jnp.sin(col_angle))

def turn_pairs(part, cosine, sine):
    quarter = part.shape[-1] // 2
    first = part[..., :quarter]
    second = part[..., quarter:]
    cosine = cosine[:, None, :]
    sine = sine[:, None, :]
    return jnp.concatenate([first * cosine - second * sine, second * cosine + first * sine], axis=-1)

def prepare(raw, gain, tables):
    count = raw.shape[0]
    heads = gain.shape[0]
    values = raw.astype(jnp.float32).reshape(count, heads, HD)
    scaled = values * lax.rsqrt(lax.optimization_barrier(jnp.mean(values * values, axis=-1, keepdims=True)) + 1e-06)
    scaled = scaled * gain.astype(jnp.float32)[None, :, :]
    half = HD // 2
    row_cos, row_sin, col_cos, col_sin = tables
    turned = jnp.concatenate([turn_pairs(scaled[..., :half], row_cos, row_sin), turn_pairs(scaled[..., half:], col_cos, col_sin)], axis=-1)
    return turned.astype(jnp.bfloat16)

def reference(tokens, query_weight, key_weight, value_weight, out_weight, query_gain, key_gain):
    count = tokens.shape[0]
    query_raw = jnp.dot(tokens, query_weight, preferred_element_type=jnp.float32).astype(jnp.bfloat16)
    key_raw = jnp.dot(tokens, key_weight, preferred_element_type=jnp.float32).astype(jnp.bfloat16)
    values = jnp.dot(tokens, value_weight, preferred_element_type=jnp.float32).astype(jnp.bfloat16)
    tables = angle_tables(count)
    queries = prepare(query_raw, query_gain, tables)
    keys = prepare(key_raw, key_gain, tables)
    share = HEADS // KV_HEADS
    key_float = keys.astype(jnp.float32)
    value_float = values.reshape(count, KV_HEADS, HD).astype(jnp.float32)
    block_len = math.gcd(count, 128)
    blocks = queries.reshape(count // block_len, block_len, KV_HEADS, share, HD)

    def one_block(query_block):
        scores = jnp.einsum('qhgd,khd->hgqk', query_block.astype(jnp.float32), key_float, precision=lax.Precision.HIGHEST) * HD ** (-0.5)
        row_max = lax.optimization_barrier(jnp.max(scores, axis=-1))
        expo = jnp.exp(scores - row_max[..., None])
        totals = lax.optimization_barrier(jnp.sum(expo, axis=-1))
        weights = lax.optimization_barrier(expo.astype(jnp.bfloat16)).astype(jnp.float32)
        summed = jnp.einsum('hgqk,khd->qhgd', weights, value_float, precision=lax.Precision.HIGHEST)
        attended = summed / jnp.transpose(totals, (2, 0, 1))[..., None]
        log_block = (row_max + jnp.log(totals)).reshape(HEADS, block_len)
        return (attended.astype(jnp.bfloat16).reshape(block_len, HEADS * HD), log_block)
    attended, log_blocks = lax.map(one_block, blocks)
    attended = attended.reshape(count, HEADS * HD)
    log_sums = jnp.transpose(log_blocks, (1, 0, 2)).reshape(HEADS, count)
    group_width = HEADS // N_TP * HD
    total = jnp.zeros((count, D), jnp.float32)
    for group in range(N_TP):
        lo = group * group_width
        partial_sum = jnp.dot(attended[:, lo:lo + group_width], out_weight[lo:lo + group_width], preferred_element_type=jnp.float32).astype(jnp.bfloat16)
        total = total + partial_sum.astype(jnp.float32)
    return (total.astype(jnp.bfloat16), log_sums)
```

```python
import functools
import math

import jax
import jax.numpy as jnp
from jax import lax
from jax.experimental import pallas as pl
from jax.experimental.pallas import tpu as pltpu
from jax.sharding import PartitionSpec as P

GRID_W = 64
ROPE_BASE = 10000.0
EPS = 1e-06
LOG2E = math.log2(math.e)
LN2 = math.log(2.0)
ONES = 16
TILE = 256
AHEAD = 3
BEHIND = 3
LINES = 4
SUBS = 4
MESH = pl.DeviceIdType.MESH
F32 = jnp.float32
BF16 = jnp.bfloat16


def prepare(x, gain, tables):
    quarter = x.shape[0] // 4
    x = x * lax.rsqrt(jnp.mean(x * x, axis=0, keepdims=True) + EPS) * gain
    a, b, c, d = (x[i * quarter : (i + 1) * quarter] for i in range(4))
    row_cos, row_sin, col_cos, col_sin = tables
    return jnp.concatenate(
        [
            a * row_cos - b * row_sin,
            b * row_cos + a * row_sin,
            c * col_cos - d * col_sin,
            d * col_cos + c * col_sin,
        ],
        axis=0,
    )


def angle_tables(place, quarter):
    order = lax.broadcasted_iota(jnp.int32, (quarter, place.shape[1]), 0).astype(F32)
    freq = jnp.exp(order * (-math.log(ROPE_BASE) / quarter))
    shift = GRID_W.bit_length() - 1
    row = lax.shift_right_logical(place, shift).astype(F32) * freq
    col = jnp.bitwise_and(place, GRID_W - 1).astype(F32) * freq
    return (jnp.cos(row), jnp.sin(row), jnp.cos(col), jnp.sin(col))


def kernel(
    n_sp,
    n_tp,
    sizes,
    tok_hbm,
    wq_hbm,
    wk_hbm,
    wv_hbm,
    wo_hbm,
    qg_hbm,
    kg_hbm,
    mixed_ref,
    log_ref,
    tok,
    wall,
    wkv,
    wo,
    qg,
    kg,
    gains,
    raw,
    tabs,
    tabs_late,
    queries,
    kv_early,
    kv_late,
    top,
    acc,
    att_out,
    att_in,
    res,
    local_sem,
    tok_send,
    tok_recv,
    wo_send,
    wo_recv,
    kv_send,
    kv_recv,
    att_send,
    att_recv,
):
    sp = lax.axis_index("sp")
    tp = lax.axis_index("tp")
    pairs = n_tp // 2
    cols = n_sp // 2
    pair, core = tp // 2, tp % 2
    mate = pair * 2 + (1 - core)
    col, side = sp // 2, sp % 2
    other = col * 2 + (1 - side)

    def near_place(k):
        place, bit = col, 1
        while bit < cols:
            if k & bit:
                place = place + bit * (1 - 2 * ((col // bit) % 2))
            bit *= 2
        return place

    beside = near_place(1) * 2 + side
    rows = tok.shape[2]
    heads, width = qg.shape
    kv_heads = kg.shape[0]
    share = heads // kv_heads
    span = 2 * rows
    count = rows * n_tp
    query_cols = wq_hbm.shape[1]
    kv_cols = wk_hbm.shape[0]
    group = wo.shape[2]
    chunks = len(sizes)
    starts = [sum(sizes[:c]) for c in range(chunks)]
    quarter = width // 4

    def across(i):
        return lax.rem(pair + i, pairs) * 2 + core

    loads = [
        pltpu.make_async_copy(src, dst, local_sem.at[i])
        for i, src, dst in (
            (0, tok_hbm, tok.at[0, core]),
            (1, wk_hbm, wkv.at[0:kv_cols]),
            (1, wv_hbm, wkv.at[kv_cols:]),
            (1, wq_hbm, wall.at[:, 0:query_cols]),
            (2, qg_hbm, qg),
            (3, kg_hbm, kg),
            (4, wo_hbm, wo.at[0, core]),
        )
    ]
    for load in loads:
        load.start()

    barrier = pltpu.get_barrier_semaphore()
    peers = 0
    for i in range(1, n_tp):
        pl.semaphore_signal(barrier, inc=1, device_id={"tp": lax.rem(tp + i, n_tp)}, device_id_type=MESH)
        peers += 1
    pl.semaphore_signal(barrier, inc=1, device_id={"sp": other}, device_id_type=MESH)
    peers += 1
    for i in range(1, cols):
        peer = lax.rem(col + i, cols) * 2 + side
        pl.semaphore_signal(barrier, inc=1, device_id={"sp": peer}, device_id_type=MESH)
        peers += 1
    pl.semaphore_wait(barrier, peers)

    def send(src, dst, send_sem, recv_sem, where):
        return pltpu.make_async_remote_copy(
            src_ref=src,
            dst_ref=dst,
            send_sem=send_sem,
            recv_sem=recv_sem,
            device_id=where,
            device_id_type=MESH,
        )

    def wait_sent(spot, sem):
        send(spot, spot, sem, tok_recv.at[0], {"tp": mate}).wait_send()

    def wait_here(spot, sem):
        send(spot, spot, tok_send.at[0], sem, {"tp": mate}).wait_recv()

    def rows_of(c):
        return slice(starts[c], starts[c] + sizes[c])

    def tok_sem(which, slot, c):
        return tok_recv.at[(slot * 2 + which) * chunks + c]

    def token_over(i, c):
        slot = pairs - i
        return send(
            tok_hbm.at[rows_of(c)],
            tok.at[slot, core, rows_of(c)],
            tok_send.at[2 * i],
            tok_sem(0, slot, c),
            {"tp": across(i)},
        )

    def token_on(slot, c):
        spot = tok.at[slot, core, rows_of(c)]
        return send(spot, spot, tok_send.at[2 * slot + 1], tok_sem(1, slot, c), {"tp": mate})

    for c in range(chunks):
        for i in range(1, pairs):
            token_over(i, c).start()
    send(tok_hbm, tok.at[0, core], tok_send.at[0], tok_recv.at[0], {"tp": mate}).start()

    def tokens_sent():
        for n in range(2 * pairs):
            if n != 1:
                wait_sent(tok.at[0, 0], tok_send.at[n])

    sub_rows = group // (4 * SUBS)
    shares = [(way, h) for h in range(SUBS) for way in (1, 0)]
    sides = (side, col % 2)
    friends = (other, beside)

    def wo_rows(way, whose, h):
        at = (2 * way + whose) * SUBS + h
        return pl.ds(pl.multiple_of(at * sub_rows, sub_rows), sub_rows)

    def wo_sem(slot, own, way, h):
        return wo_recv.at[slot, (own * 2 + way) * SUBS + h]

    def wo_over(i, way, h):
        slot = pairs - i
        at = wo_rows(way, sides[way], h)
        return send(
            wo_hbm.at[at], wo.at[slot, core, at], wo_send.at[i, 0], wo_sem(slot, 0, way, h), {"tp": across(i)}
        )

    def wo_on(slot, way, h):
        spot = wo.at[slot, core, wo_rows(way, sides[way], h)]
        return send(spot, spot, wo_send.at[slot, 1], wo_sem(slot, 1, way, h), {"sp": friends[way]})

    def wo_give(slot, way, whose, h):
        spot = wo.at[slot, core, wo_rows(way, whose, h)]
        return send(spot, spot, wo_send.at[slot, 2], wo_recv.at[slot, 4 * SUBS], {"tp": mate})

    send(wo_hbm, wo.at[0, core], wo_send.at[0, 0], wo_recv.at[0, 0], {"tp": mate}).start()
    for way, h in shares:
        for i in range(1, pairs):
            wo_over(i, way, h).start()

    def wo_pass(start, stop):
        for way, h in shares[start:stop]:
            for slot in range(1, pairs):
                wait_here(wo.at[slot, core, wo_rows(way, sides[way], h)], wo_sem(slot, 0, way, h))
                wo_on(slot, way, h).start()
                wo_give(slot, way, sides[way], h).start()

    def wo_take(start, stop):
        for way, h in shares[start:stop]:
            for slot in range(1, pairs):
                wait_here(wo.at[slot, core, wo_rows(way, 1 - sides[way], h)], wo_sem(slot, 1, way, h))
                wo_give(slot, way, 1 - sides[way], h).start()

    def wo_last():
        for slot in range(1, pairs):
            wait_here(wo.at[slot, 1 - core], wo_recv.at[slot, 4 * SUBS])

    def wo_sent():
        wait_sent(wo.at[0, 0], wo_send.at[0, 0])
        for slot in range(1, pairs):
            for lane in range(2):
                wait_sent(wo.at[0, 0, 0 : group // 2], wo_send.at[slot, lane])
            wait_sent(wo.at[0, 0], wo_send.at[slot, 2])

    def part_of(slot):
        return lax.rem(pair + slot, pairs)

    for slot in range(pairs):
        lane = lax.broadcasted_iota(jnp.int32, (quarter, span), 1)
        first = sp * count + part_of(slot) * span
        for n, table in enumerate(angle_tables(first + lane, quarter)):
            tabs[slot, n] = table
    for slot in range(1, pairs):
        for c in range(chunks):
            lane = lax.broadcasted_iota(jnp.int32, (quarter, 2 * sizes[c]), 1)
            lane = jnp.where(lane < sizes[c], lane, lane + (rows - sizes[c]))
            first = sp * count + part_of(slot) * span + starts[c]
            for n, table in enumerate(angle_tables(first + lane, quarter)):
                tabs_late[(slot - 1) * chunks + c][n] = table
    top[...] = jnp.full_like(top, -1e30)
    acc[...] = jnp.zeros_like(acc)
    pltpu.make_async_copy(wall, wall, local_sem.at[1]).wait()
    for load in loads[4:6]:
        load.wait()
    wall[:, query_cols:] = jnp.transpose(wkv[...])
    gains[...] = jnp.zeros_like(gains)
    gains[0:heads, 0:width] = qg[...].astype(F32) * (LOG2E * width ** (-0.5))
    gains[heads : heads + kv_heads, 0:width] = kg[...].astype(F32)
    turned_gains = jnp.transpose(gains[...])
    kv_rows = kv_heads * width

    def make_kv(x, tables, put):
        turned = jnp.transpose(x[:, 0:kv_rows])
        for g in range(kv_heads):
            gain = turned_gains[0:width, heads + g : heads + g + 1]
            keys = prepare(turned[g * width : (g + 1) * width], gain, tables)
            put(slice(g * width, (g + 1) * width), jnp.transpose(keys).astype(BF16))
        put(slice(kv_rows, 2 * kv_rows), x[:, kv_rows:].astype(BF16))

    def make_queries(slot):
        turned = jnp.transpose(raw[slot])
        tables = tuple(tabs[slot, n] for n in range(4))
        for g in range(kv_heads):
            made = []
            for h in range(g * share, (g + 1) * share):
                q = prepare(turned[h * width : (h + 1) * width], turned_gains[0:width, h : h + 1], tables)
                made.append(q.astype(BF16))
            queries[slot, g] = jnp.concatenate(made, axis=1)

    def kv_ref(unit):
        return kv_early if unit == 0 else kv_late[unit - 1]

    def kv_copy(unit, block, number, where):
        spot = kv_ref(unit).at[block]
        return send(spot, spot, kv_send.at[unit], kv_recv.at[unit, number], {"sp": where})

    def mirror(k):
        return cols + (0 if k < 2 else 1)

    def send_kv(unit):
        kv_copy(unit, sp, mirror(0), other).start()
        for k in range(1, cols):
            kv_copy(unit, sp, k, near_place(k) * 2 + side).start()

    def forward_kv(unit, start, stop):
        for k in range(start, stop):
            block = near_place(k) * 2 + side
            kv_copy(unit, block, k, other).wait_recv()
            kv_copy(unit, block, mirror(k), other).start()

    def mirrored_kv(unit, n):
        many = 2 if n == 0 else cols - 2
        wait_here(kv_ref(unit).at[0:many], kv_recv.at[unit, cols + n])

    def sent_kv(unit):
        wait_sent(kv_ref(unit).at[0 : n_sp - 1], kv_send.at[unit])

    loads[0].wait()
    wait_here(tok.at[0, 1 - core], tok_recv.at[0])
    depth = tok.shape[3]
    x = jnp.dot(tok[0].reshape(span, depth), wall[:, query_cols:], preferred_element_type=F32)

    def put_early(at, value):
        kv_early[sp, :, at] = value

    make_kv(x, tuple(tabs[0, n] for n in range(4)), put_early)
    send_kv(0)
    raw[0] = jnp.dot(tok[0].reshape(span, depth), wall[:, 0:query_cols], preferred_element_type=F32)
    make_queries(0)

    tiles = share * span // TILE

    def attend(loaders, slots):
        items = [(n, slot, g, t) for n in range(len(loaders)) for slot in slots for g in range(kv_heads) for t in range(tiles)]
        held = {}
        for n, load in enumerate(loaders):
            block = load()
            turned = jnp.transpose(block)
            ones = jnp.ones((ONES, block.shape[0]), BF16)
            for g in range(kv_heads):
                keys = block[:, g * width : (g + 1) * width]
                values = turned[kv_rows + g * width : kv_rows + (g + 1) * width]
                held[n, g] = (keys, jnp.concatenate([values, ones], axis=0))
        scores, weights = {}, {}

        def spot(i):
            _, slot, g, t = items[i]
            return (slot * kv_heads + g) * tiles + t

        def score(i):
            n, slot, g, t = items[i]
            q = queries[slot, g, :, t * TILE : (t + 1) * TILE]
            scores[i] = jnp.dot(held[n, g][0], q, preferred_element_type=F32)

        def soften(i):
            s = scores.pop(i)
            at = spot(i)
            old = top[at]
            new = jnp.maximum(old, jnp.max(s, axis=0, keepdims=True))
            top[at] = new
            weights[i] = (jnp.exp2(s - new).astype(BF16), jnp.exp2(old - new))

        def gather(i):
            n, slot, g, t = items[i]
            w, scale = weights.pop(i)
            at = spot(i)
            acc[at] = acc[at] * scale + jnp.dot(held[n, g][1], w, preferred_element_type=F32)

        total = len(items)
        for i in range(min(AHEAD, total)):
            score(i)
        for i in range(total):
            if i + AHEAD < total:
                score(i + AHEAD)
            if i >= BEHIND:
                gather(i - BEHIND)
            soften(i)
        for i in range(max(total - BEHIND, 0), total):
            gather(i)

    def early(k):
        place = near_place(k)
        return lambda: kv_early[pl.ds(pl.multiple_of(place * 2, 2), 2)].reshape(2 * span, 2 * kv_rows)

    def late_line(unit, k, way):
        def load():
            return jnp.concatenate([kv_late[unit - 1][(k + n) * 2 + way] for n in range(LINES)], axis=0)

        return load

    late_units = [1 + (slot - 1) * chunks + c for slot in range(1, pairs) for c in range(chunks)]
    late_order = [(slot, c) for c in range(chunks) for slot in range(1, pairs)]

    def token_first(slot, c):
        wait_here(tok.at[slot, core, rows_of(c)], tok_sem(0, slot, c))
        token_on(slot, c).start()

    def token_second(slot, c):
        unit = 1 + (slot - 1) * chunks + c
        wait_here(tok.at[slot, 1 - core, rows_of(c)], tok_sem(1, slot, c))
        piece = tok[slot, :, rows_of(c)].reshape(2 * sizes[c], depth)
        x = jnp.dot(piece, wall[:, query_cols:], preferred_element_type=F32)

        def put_late(at, value):
            kv_late[unit - 1][sp, :, at] = value

        make_kv(x, tuple(tabs_late[unit - 1][n] for n in range(4)), put_late)
        send_kv(unit)
        x = jnp.dot(piece, wall[:, 0:query_cols], preferred_element_type=F32)
        for which in range(2):
            at = slice(which * rows + starts[c], which * rows + starts[c] + sizes[c])
            raw[slot, at] = x[which * sizes[c] : (which + 1) * sizes[c]]

    def attend_early(slots, start, stop):
        for k in range(start, stop, LINES):
            attend([early(n) for n in range(k, min(k + LINES, stop))], slots)

    def attend_late(unit, way):
        for k in range(0, cols, LINES):
            attend([late_line(unit, k, way)], everyone)

    remote = list(range(1, pairs))
    everyone = remote + [0]
    firsts, last = late_units[:-1], late_units[-1]
    forward_kv(0, 1, 3)
    for slot, c in late_order[:1]:
        token_first(slot, c)
    forward_kv(0, 3, cols)
    for slot, c in late_order[:1]:
        token_second(slot, c)
    for slot, c in late_order[1:-1]:
        token_first(slot, c)
        token_second(slot, c)
    mirrored_kv(0, 0)
    attend_early([0], 0, 2)
    for slot, c in late_order[-1:]:
        token_first(slot, c)
        token_second(slot, c)
    for unit in firsts:
        forward_kv(unit, 1, cols)
    for slot in remote:
        make_queries(slot)
    mirrored_kv(0, 1)
    attend_early([0], 2, cols)
    forward_kv(last, 1, 2)
    wo_pass(0, 1)
    attend_early(remote, 0, 2)
    forward_kv(last, 2, 3)
    attend_early(remote, 2, cols)
    forward_kv(last, 3, cols)
    wo_pass(1, 3)
    for unit in firsts:
        attend_late(unit, side)
    wo_pass(3, 4)
    for unit in firsts:
        mirrored_kv(unit, 0)
        mirrored_kv(unit, 1)
        attend_late(unit, 1 - side)
    wo_pass(4, 5)
    attend_late(last, side)
    wo_pass(5, 6)
    mirrored_kv(last, 0)
    mirrored_kv(last, 1)
    attend_late(last, 1 - side)
    wo_pass(6, 7)

    logs = {}

    def att_copy(slot, which):
        there = 0 if slot == 0 else pairs - slot
        return send(
            att_out.at[slot, which],
            att_in.at[there, core],
            att_send.at[slot],
            att_recv.at[there],
            {"tp": part_of(slot) * 2 + which},
        )

    for slot in everyone:
        turned = []
        for g in range(kv_heads):
            made, sums = [], []
            for t in range(tiles):
                at = (slot * kv_heads + g) * tiles + t
                total = acc[at, width : width + 1, :]
                made.append((acc[at, 0:width, :] * (1.0 / total)).astype(BF16))
                sums.append((top[at] + jnp.log2(total)) * LN2)
            turned.append(jnp.transpose(jnp.concatenate(made, axis=1)))
            logs[slot, g] = jnp.concatenate(sums, axis=1)
        for which in range(2):
            piece = jnp.concatenate(
                [
                    turned[g][h * span + which * rows : h * span + (which + 1) * rows]
                    for g in range(kv_heads)
                    for h in range(share)
                ],
                axis=1,
            )
            if slot:
                att_out[slot, which] = piece
                att_copy(slot, which).start()
            else:

                @pl.when(core == which)
                def _():
                    att_in[0, which] = piece

                @pl.when(core != which)
                def _():
                    att_out[0, which] = piece

    att_copy(0, 1 - core).start()
    wo_pass(7, 8)
    for g in range(kv_heads):
        for h in range(share):
            lines = [logs[slot, g][:, h * span : (h + 1) * span] for slot in range(pairs)]
            for part in range(pairs):
                line = lines[0]
                for slot in range(1, pairs):
                    line = jnp.where(part_of(slot) == part, lines[slot], line)
                log_ref[g * share + h : g * share + h + 1, part * span : (part + 1) * span] = line

    wo_take(0, 4)
    loads[6].wait()
    wait_here(wo.at[0, 1 - core], wo_recv.at[0, 0])

    model = wo.shape[3]
    step_cols = 512
    wait_here(att_in.at[0, 1 - core], att_recv.at[0])
    for n in range(model // step_cols):
        at = slice(n * step_cols, (n + 1) * step_cols)
        res[:, at] = jnp.dot(att_in[0, 0], wo[0, 0, :, at], preferred_element_type=F32) + jnp.dot(
            att_in[0, 1], wo[0, 1, :, at], preferred_element_type=F32
        )
    wo_take(4, 8)
    for unit in [0] + late_units:
        sent_kv(unit)
    tokens_sent()
    for slot in range(1, pairs):
        wait_here(att_in.at[slot], att_recv.at[slot])
    wo_last()
    for n in range(model // step_cols):
        at = slice(n * step_cols, (n + 1) * step_cols)
        total = res[:, at]
        for slot in range(1, pairs):
            for which in range(2):
                total = total + jnp.dot(att_in[slot, which], wo[slot, which, :, at], preferred_element_type=F32)
        mixed_ref[:, at] = total.astype(BF16)

    wait_sent(att_out.at[0, 0], att_send.at[0])
    for slot in range(1, pairs):
        wait_sent(att_out.at[slot], att_send.at[slot])
    wo_sent()


def body(n_sp, n_tp, tokens, query_weight, key_weight, value_weight, out_weight, query_gain, key_gain):
    rows, depth = tokens.shape
    query_cols = query_weight.shape[1]
    kv_cols = key_weight.shape[1]
    heads, width = query_gain.shape
    kv_heads = key_gain.shape[0]
    group, model = out_weight.shape
    count = rows * n_tp
    pairs, cols = n_tp // 2, n_sp // 2
    sizes = (rows * 2 // 3, rows - rows * 2 // 3)
    chunks = len(sizes)
    span = 2 * rows
    units = 1 + (pairs - 1) * chunks
    spots = pairs * heads * span // TILE
    any_space = pl.BlockSpec(memory_space=pl.ANY)
    vmem = pl.BlockSpec(memory_space=pltpu.VMEM)
    dma = pltpu.SemaphoreType.DMA
    return pl.pallas_call(
        functools.partial(kernel, n_sp, n_tp, sizes),
        out_shape=(
            pltpu.VMEM((rows, model), BF16),
            pltpu.VMEM((heads, count), F32),
        ),
        in_specs=[any_space] * 7,
        out_specs=(vmem, vmem),
        scratch_shapes=[
            pltpu.VMEM((pairs, 2, rows, depth), BF16),
            pltpu.VMEM((depth, query_cols + 2 * kv_cols), BF16),
            pltpu.VMEM((2 * kv_cols, depth), BF16),
            pltpu.VMEM((pairs, 2, group, model), BF16),
            pltpu.VMEM((heads, width), BF16),
            pltpu.VMEM((kv_heads, width), BF16),
            pltpu.VMEM((128, 128), F32),
            pltpu.VMEM((pairs, span, query_cols), F32),
            pltpu.VMEM((pairs, 4, width // 4, span), F32),
            [pltpu.VMEM((4, width // 4, 2 * size), F32) for size in sizes] * (pairs - 1),
            pltpu.VMEM((pairs, kv_heads, width, heads // kv_heads * span), BF16),
            pltpu.VMEM((n_sp, span, 2 * kv_cols), BF16),
            [pltpu.VMEM((n_sp, 2 * size, 2 * kv_cols), BF16) for size in sizes] * (pairs - 1),
            pltpu.VMEM((spots, 1, TILE), F32),
            pltpu.VMEM((spots, width + ONES, TILE), F32),
            pltpu.VMEM((pairs, 2, rows, group), BF16),
            pltpu.VMEM((pairs, 2, rows, group), BF16),
            pltpu.VMEM((rows, model), F32),
            dma((5,)),
            dma((2 * pairs,)),
            dma((2 * pairs * chunks,)),
            dma((pairs, 3)),
            dma((pairs, 4 * SUBS + 1)),
            dma((units,)),
            dma((units, cols + 2)),
            dma((pairs,)),
            dma((pairs,)),
        ],
        compiler_params=pltpu.CompilerParams(
            collective_id=0, has_side_effects=True, vmem_limit_bytes=60 * 1024 * 1024
        ),
        name="attention",
    )(tokens, query_weight, key_weight.T, value_weight.T, out_weight, query_gain, key_gain)


def solution(mesh):
    return jax.shard_map(
        functools.partial(body, mesh.shape["sp"], mesh.shape["tp"]),
        mesh=mesh,
        in_specs=(
            P(("sp", "tp"), None),
            P(None, "tp"),
            P(None, "tp"),
            P(None, "tp"),
            P("tp", None),
            P("tp", None),
            P("tp", None),
        ),
        out_specs=(P(("sp", "tp"), None), P("tp", "sp")),
        check_vma=False,
    )
```

```python
import functools
import math

import jax
import jax.numpy as jnp
from jax import lax
from jax.experimental import pallas as pl
from jax.experimental.pallas import tpu as pltpu
from jax.sharding import PartitionSpec as P

GRID_W = 64
ROPE_BASE = 10000.0
EPS = 1e-06
LOG2E = math.log2(math.e)
LN2 = math.log(2.0)
ONES = 16
TILE = 256
AHEAD = 3
BEHIND = 3
LINES = 4
UNITS = 16
ACROSS = 6
ASIDE = 5
MESH = pl.DeviceIdType.MESH
F32 = jnp.float32
BF16 = jnp.bfloat16


def prepare(x, gain, tables):
    quarter = x.shape[0] // 4
    x = x * lax.rsqrt(jnp.mean(x * x, axis=0, keepdims=True) + EPS) * gain
    a, b, c, d = (x[i * quarter : (i + 1) * quarter] for i in range(4))
    row_cos, row_sin, col_cos, col_sin = tables
    return jnp.concatenate(
        [
            a * row_cos - b * row_sin,
            b * row_cos + a * row_sin,
            c * col_cos - d * col_sin,
            d * col_cos + c * col_sin,
        ],
        axis=0,
    )


def angle_tables(place, quarter):
    order = lax.broadcasted_iota(jnp.int32, (quarter, place.shape[1]), 0).astype(F32)
    freq = jnp.exp(order * (-math.log(ROPE_BASE) / quarter))
    shift = GRID_W.bit_length() - 1
    row = lax.shift_right_logical(place, shift).astype(F32) * freq
    col = jnp.bitwise_and(place, GRID_W - 1).astype(F32) * freq
    return (jnp.cos(row), jnp.sin(row), jnp.cos(col), jnp.sin(col))


def kernel(
    n_sp,
    n_tp,
    sizes,
    tok_hbm,
    wq_hbm,
    wk_hbm,
    wv_hbm,
    wo_hbm,
    qg_hbm,
    kg_hbm,
    mixed_ref,
    log_ref,
    tok,
    wall,
    wkv,
    wo,
    qg,
    kg,
    gains,
    raw,
    tabs,
    tabs_late,
    queries,
    kv_early,
    kv_late,
    top,
    acc,
    att_out,
    att_in,
    res,
    local_sem,
    tok_send,
    tok_recv,
    wo_send,
    wo_recv,
    kv_send,
    kv_recv,
    att_send,
    att_recv,
):
    sp = lax.axis_index("sp")
    tp = lax.axis_index("tp")
    pairs = n_tp // 2
    cols = n_sp // 2
    pair, core = tp // 2, tp % 2
    mate = pair * 2 + (1 - core)
    col, side = sp // 2, sp % 2
    other = col * 2 + (1 - side)

    def near_place(k):
        place, bit = col, 1
        while bit < cols:
            if k & bit:
                place = place + bit * (1 - 2 * ((col // bit) % 2))
            bit *= 2
        return place

    beside = near_place(1) * 2 + side
    rows = tok.shape[2]
    heads, width = qg.shape
    kv_heads = kg.shape[0]
    share = heads // kv_heads
    span = 2 * rows
    count = rows * n_tp
    query_cols = wq_hbm.shape[1]
    kv_cols = wk_hbm.shape[0]
    group = wo.shape[2]
    chunks = len(sizes)
    starts = [sum(sizes[:c]) for c in range(chunks)]
    quarter = width // 4

    def across(i):
        return lax.rem(pair + i, pairs) * 2 + core

    loads = [
        pltpu.make_async_copy(src, dst, local_sem.at[i])
        for i, src, dst in (
            (0, tok_hbm, tok.at[0, core]),
            (1, wk_hbm, wkv.at[0:kv_cols]),
            (1, wv_hbm, wkv.at[kv_cols:]),
            (1, wq_hbm, wall.at[:, 0:query_cols]),
            (2, qg_hbm, qg),
            (3, kg_hbm, kg),
            (4, wo_hbm, wo.at[0, core]),
        )
    ]
    for load in loads:
        load.start()

    barrier = pltpu.get_barrier_semaphore()
    peers = 0
    for i in range(1, n_tp):
        pl.semaphore_signal(barrier, inc=1, device_id={"tp": lax.rem(tp + i, n_tp)}, device_id_type=MESH)
        peers += 1
    pl.semaphore_signal(barrier, inc=1, device_id={"sp": other}, device_id_type=MESH)
    peers += 1
    for i in range(1, cols):
        peer = lax.rem(col + i, cols) * 2 + side
        pl.semaphore_signal(barrier, inc=1, device_id={"sp": peer}, device_id_type=MESH)
        peers += 1
    pl.semaphore_wait(barrier, peers)

    def send(src, dst, send_sem, recv_sem, where):
        return pltpu.make_async_remote_copy(
            src_ref=src,
            dst_ref=dst,
            send_sem=send_sem,
            recv_sem=recv_sem,
            device_id=where,
            device_id_type=MESH,
        )

    def wait_sent(spot, sem):
        send(spot, spot, sem, tok_recv.at[0], {"tp": mate}).wait_send()

    def wait_here(spot, sem):
        send(spot, spot, tok_send.at[0], sem, {"tp": mate}).wait_recv()

    def rows_of(c):
        return slice(starts[c], starts[c] + sizes[c])

    def tok_sem(which, slot, c):
        return tok_recv.at[1 + ((slot - 1) * 2 + which) * chunks + c]

    def token_over(i, c):
        slot = pairs - i
        return send(
            tok.at[0, core, rows_of(c)],
            tok.at[slot, core, rows_of(c)],
            tok_send.at[2 * i - 1],
            tok_sem(0, slot, c),
            {"tp": across(i)},
        )

    def token_on(slot, c):
        spot = tok.at[slot, core, rows_of(c)]
        return send(spot, spot, tok_send.at[2 * slot], tok_sem(1, slot, c), {"tp": mate})

    loads[0].wait()
    for c in range(chunks):
        for i in range(1, pairs):
            token_over(i, c).start()
    send(tok.at[0, core], tok.at[0, core], tok_send.at[0], tok_recv.at[0], {"tp": mate}).start()

    def tokens_sent():
        for n in range(2 * pairs - 1):
            wait_sent(tok.at[0, 0], tok_send.at[n])

    unit_rows = group // UNITS
    color = sp % 4
    colors = (color + 1 - 2 * (color % 2), (color + 2) % 4)
    color_far = 3 - color
    sides = (side, col % 2)
    friends = (other, beside)

    def ring_unit(whose, h):
        return whose * 2 + h

    def swap_unit(way, whose, h):
        return 8 + way * 4 + whose * 2 + h

    def wo_at(ref, unit):
        return ref.at[pl.ds(pl.multiple_of(unit * unit_rows, unit_rows), unit_rows)]

    def arrival(slot, number):
        return 1 + (slot - 1) * (ACROSS + 2 * ASIDE + 1) + number

    over = [(ring_unit(color, h), h) for h in range(2)]
    over += [(swap_unit(way, sides[way], h), 2 + way * 2 + h) for h in range(2) for way in (1, 0)]

    def wo_over(i, unit, number):
        slot = pairs - i
        return send(
            wo_at(wo_hbm, unit), wo_at(wo.at[slot, core], unit), wo_send.at[3 * i - 2 + 0], wo_recv.at[arrival(slot, number)], {"tp": across(i)}
        )

    def wo_aside(slot, unit, way, number):
        spot = wo_at(wo.at[slot, core], unit)
        return send(spot, spot, wo_send.at[3 * slot - 2 + 1], wo_recv.at[arrival(slot, ACROSS + way * ASIDE + number)], {"sp": friends[way]})

    def wo_got(slot, unit, number):
        spot = wo_at(wo.at[slot, core], unit)
        wait_here(spot, wo_recv.at[arrival(slot, number)])
        send(spot, spot, wo_send.at[3 * slot - 2 + 2], wo_recv.at[arrival(slot, ACROSS + 2 * ASIDE)], {"tp": mate}).start()

    send(wo_hbm, wo.at[0, core], wo_send.at[0], wo_recv.at[0], {"tp": mate}).start()
    for unit, number in over:
        for i in range(1, pairs):
            wo_over(i, unit, number).start()

    def ring_first(h):
        for slot in range(1, pairs):
            wo_got(slot, ring_unit(color, h), h)
            for way in range(2):
                wo_aside(slot, ring_unit(color, h), way, h).start()

    def ring_second(h):
        for slot in range(1, pairs):
            for way in range(2):
                wo_got(slot, ring_unit(colors[way], h), ACROSS + way * ASIDE + h)
                if way != h:
                    wo_aside(slot, ring_unit(colors[way], h), 1 - way, 4).start()

    def ring_third(h):
        for slot in range(1, pairs):
            wo_got(slot, ring_unit(color_far, h), ACROSS + h * ASIDE + 4)

    def swap_first(way, h):
        for slot in range(1, pairs):
            wo_got(slot, swap_unit(way, sides[way], h), 2 + way * 2 + h)
            wo_aside(slot, swap_unit(way, sides[way], h), way, 2 + h).start()

    def swap_second(way, h):
        for slot in range(1, pairs):
            wo_got(slot, swap_unit(way, 1 - sides[way], h), ACROSS + way * ASIDE + 2 + h)

    def wo_last():
        for slot in range(1, pairs):
            wait_here(wo.at[slot, 1 - core], wo_recv.at[arrival(slot, ACROSS + 2 * ASIDE)])

    def wo_sent():
        wait_sent(wo.at[0, 0], wo_send.at[0])
        for slot in range(1, pairs):
            wait_sent(wo.at[0, 0, 0 : ACROSS * unit_rows], wo_send.at[3 * slot - 2 + 0])
            wait_sent(wo.at[0, 0, 0 : 2 * ASIDE * unit_rows], wo_send.at[3 * slot - 2 + 1])
            wait_sent(wo.at[0, 0], wo_send.at[3 * slot - 2 + 2])

    def part_of(slot):
        return lax.rem(pair + slot, pairs)

    for slot in range(pairs):
        lane = lax.broadcasted_iota(jnp.int32, (quarter, span), 1)
        first = sp * count + part_of(slot) * span
        for n, table in enumerate(angle_tables(first + lane, quarter)):
            tabs[slot, n] = table
    for slot in range(1, pairs):
        for c in range(chunks):
            lane = lax.broadcasted_iota(jnp.int32, (quarter, 2 * sizes[c]), 1)
            lane = jnp.where(lane < sizes[c], lane, lane + (rows - sizes[c]))
            first = sp * count + part_of(slot) * span + starts[c]
            for n, table in enumerate(angle_tables(first + lane, quarter)):
                tabs_late[(slot - 1) * chunks + c][n] = table
    top[...] = jnp.full_like(top, -1e30)
    acc[...] = jnp.zeros_like(acc)
    pltpu.make_async_copy(wall, wall, local_sem.at[1]).wait()
    for load in loads[4:6]:
        load.wait()
    wall[:, query_cols:] = jnp.transpose(wkv[...])
    gains[...] = jnp.zeros_like(gains)
    gains[0:heads, 0:width] = qg[...].astype(F32) * (LOG2E * width ** (-0.5))
    gains[heads : heads + kv_heads, 0:width] = kg[...].astype(F32)
    turned_gains = jnp.transpose(gains[...])
    kv_rows = kv_heads * width

    def make_kv(x, tables, put):
        turned = jnp.transpose(x[:, 0:kv_rows])
        for g in range(kv_heads):
            gain = turned_gains[0:width, heads + g : heads + g + 1]
            keys = prepare(turned[g * width : (g + 1) * width], gain, tables)
            put(slice(g * width, (g + 1) * width), jnp.transpose(keys).astype(BF16))
        put(slice(kv_rows, 2 * kv_rows), x[:, kv_rows:].astype(BF16))

    def make_queries(slot):
        turned = jnp.transpose(raw[slot])
        tables = tuple(tabs[slot, n] for n in range(4))
        for g in range(kv_heads):
            made = []
            for h in range(g * share, (g + 1) * share):
                q = prepare(turned[h * width : (h + 1) * width], turned_gains[0:width, h : h + 1], tables)
                made.append(q.astype(BF16))
            queries[slot, g] = jnp.concatenate(made, axis=1)

    def kv_ref(unit):
        return kv_early if unit == 0 else kv_late[unit - 1]

    def kv_copy(unit, block, number, where):
        spot = kv_ref(unit).at[block]
        return send(spot, spot, kv_send.at[unit], kv_recv.at[unit, number], {"sp": where})

    def send_kv(unit):
        kv_copy(unit, sp, 0 if unit else cols, other).start()
        for k in range(1, cols):
            kv_copy(unit, sp, k, near_place(k) * 2 + side).start()

    def forward_kv(unit, start, stop):
        for k in range(start, stop):
            block = near_place(k) * 2 + side
            kv_copy(unit, block, k, other).wait_recv()
            kv_copy(unit, block, 0, other).start()

    def mirrored_kv(unit):
        if unit == 0:
            wait_here(kv_early.at[0 : cols - 1], kv_recv.at[0, 0])
        else:
            wait_here(kv_ref(unit).at[0:cols], kv_recv.at[unit, 0])

    def sent_kv(unit):
        wait_sent(kv_ref(unit).at[0 : n_sp - 1], kv_send.at[unit])

    wait_here(tok.at[0, 1 - core], tok_recv.at[0])
    depth = tok.shape[3]
    x = jnp.dot(tok[0].reshape(span, depth), wall[:, query_cols:], preferred_element_type=F32)

    def put_early(at, value):
        kv_early[sp, :, at] = value

    make_kv(x, tuple(tabs[0, n] for n in range(4)), put_early)
    send_kv(0)
    raw[0] = jnp.dot(tok[0].reshape(span, depth), wall[:, 0:query_cols], preferred_element_type=F32)
    make_queries(0)

    tiles = share * span // TILE

    def attend(loaders, slots):
        items = [(n, slot, g, t) for n in range(len(loaders)) for slot in slots for g in range(kv_heads) for t in range(tiles)]
        held = {}
        for n, load in enumerate(loaders):
            block = load()
            turned = jnp.transpose(block)
            ones = jnp.ones((ONES, block.shape[0]), BF16)
            for g in range(kv_heads):
                keys = block[:, g * width : (g + 1) * width]
                values = turned[kv_rows + g * width : kv_rows + (g + 1) * width]
                held[n, g] = (keys, jnp.concatenate([values, ones], axis=0))
        scores, weights = {}, {}

        def spot(i):
            _, slot, g, t = items[i]
            return (slot * kv_heads + g) * tiles + t

        def score(i):
            n, slot, g, t = items[i]
            q = queries[slot, g, :, t * TILE : (t + 1) * TILE]
            scores[i] = jnp.dot(held[n, g][0], q, preferred_element_type=F32)

        def soften(i):
            s = scores.pop(i)
            at = spot(i)
            old = top[at]
            new = jnp.maximum(old, jnp.max(s, axis=0, keepdims=True))
            top[at] = new
            weights[i] = (jnp.exp2(s - new).astype(BF16), jnp.exp2(old - new))

        def gather(i):
            n, slot, g, t = items[i]
            w, scale = weights.pop(i)
            at = spot(i)
            acc[at] = acc[at] * scale + jnp.dot(held[n, g][1], w, preferred_element_type=F32)

        total = len(items)
        for i in range(min(AHEAD, total)):
            score(i)
        for i in range(total):
            if i + AHEAD < total:
                score(i + AHEAD)
            if i >= BEHIND:
                gather(i - BEHIND)
            soften(i)
        for i in range(max(total - BEHIND, 0), total):
            gather(i)

    def early_blocks(*blocks):
        def load():
            return jnp.concatenate([kv_early[near_place(k) * 2 + way] for k, way in blocks], axis=0)

        return load

    def late_line(unit, k, way):
        def load():
            return jnp.concatenate([kv_late[unit - 1][(k + n) * 2 + way] for n in range(LINES)], axis=0)

        return load

    late_units = [1 + (slot - 1) * chunks + c for slot in range(1, pairs) for c in range(chunks)]
    late_order = [(slot, c) for c in range(chunks) for slot in range(1, pairs)]

    def token_first(slot, c):
        wait_here(tok.at[slot, core, rows_of(c)], tok_sem(0, slot, c))
        token_on(slot, c).start()

    def token_second(slot, c):
        unit = 1 + (slot - 1) * chunks + c
        wait_here(tok.at[slot, 1 - core, rows_of(c)], tok_sem(1, slot, c))
        piece = tok[slot, :, rows_of(c)].reshape(2 * sizes[c], depth)
        x = jnp.dot(piece, wall[:, query_cols:], preferred_element_type=F32)

        def put_late(at, value):
            kv_late[unit - 1][sp, :, at] = value

        make_kv(x, tuple(tabs_late[unit - 1][n] for n in range(4)), put_late)
        send_kv(unit)
        x = jnp.dot(piece, wall[:, 0:query_cols], preferred_element_type=F32)
        for which in range(2):
            at = slice(which * rows + starts[c], which * rows + starts[c] + sizes[c])
            raw[slot, at] = x[which * sizes[c] : (which + 1) * sizes[c]]

    def attend_early(slots, ways):
        for k in range(0, cols, LINES):
            attend([early_blocks((k + n, way), (k + n + 1, way)) for way in ways for n in range(0, LINES, 2)], slots)

    def attend_late(units, ways, slots):
        for k in range(0, cols, LINES):
            attend([late_line(unit, k, way) for unit in units for way in ways], slots)

    remote = list(range(1, pairs))
    everyone = remote + [0]
    firsts, last = late_units[:-1], late_units[-1]
    wait_here(kv_early.at[0], kv_recv.at[0, cols])
    attend([early_blocks((0, side), (0, 1 - side))], [0])
    forward_kv(0, 1, 3)
    for slot, c in late_order[:1]:
        token_first(slot, c)
    forward_kv(0, 3, cols)
    for slot, c in late_order[:1]:
        token_second(slot, c)
    for slot, c in late_order[1:-1]:
        token_first(slot, c)
        token_second(slot, c)
    attend([early_blocks(*((n, side) for n in range(1, LINES)))], [0])
    for slot, c in late_order[-1:]:
        token_first(slot, c)
    for unit in firsts:
        forward_kv(unit, 1, 2)
    for slot, c in late_order[-1:]:
        token_second(slot, c)
    for unit in firsts:
        forward_kv(unit, 2, cols)
    ring_first(0)
    for slot in remote:
        make_queries(slot)
    mirrored_kv(0)
    attend([early_blocks(*((n, 1 - side) for n in range(1, LINES)))], [0])
    for k in range(LINES, cols, LINES):
        attend([early_blocks((k + n, way), (k + n + 1, way)) for way in (side, 1 - side) for n in range(0, LINES, 2)], [0])
    ring_first(1)
    forward_kv(last, 1, 2)
    swap_first(1, 0)
    attend_early(remote, [side])
    forward_kv(last, 2, cols)
    attend_early(remote, [1 - side])
    swap_first(0, 0)
    for unit in firsts:
        mirrored_kv(unit)
    attend_late(firsts, [side, 1 - side], remote)
    swap_first(1, 1)
    ring_second(0)
    attend_late(firsts, [side, 1 - side], [0])
    swap_first(0, 1)
    ring_second(1)
    swap_second(1, 0)
    mirrored_kv(last)
    attend_late([last], [side, 1 - side], remote)

    logs = {}

    def att_copy(slot, which):
        there = 0 if slot == 0 else pairs - slot
        return send(
            att_out.at[slot, which],
            att_in.at[there, core],
            att_send.at[slot],
            att_recv.at[there],
            {"tp": part_of(slot) * 2 + which},
        )

    def finish(slot):
        turned = []
        for g in range(kv_heads):
            made, sums = [], []
            for t in range(tiles):
                at = (slot * kv_heads + g) * tiles + t
                total = acc[at, width : width + 1, :]
                made.append((acc[at, 0:width, :] * (1.0 / total)).astype(BF16))
                sums.append((top[at] + jnp.log2(total)) * LN2)
            turned.append(jnp.transpose(jnp.concatenate(made, axis=1)))
            logs[slot, g] = jnp.concatenate(sums, axis=1)
        for which in range(2):
            piece = jnp.concatenate(
                [
                    turned[g][h * span + which * rows : h * span + (which + 1) * rows]
                    for g in range(kv_heads)
                    for h in range(share)
                ],
                axis=1,
            )
            if slot:
                att_out[slot, which] = piece
                att_copy(slot, which).start()
            else:

                @pl.when(core == which)
                def _():
                    att_in[0, which] = piece

                @pl.when(core != which)
                def _():
                    att_out[0, which] = piece

    for slot in remote:
        finish(slot)
    attend_late([last], [side, 1 - side], [0])
    finish(0)
    att_copy(0, 1 - core).start()
    swap_second(0, 0)
    ring_third(0)
    for g in range(kv_heads):
        for h in range(share):
            lines = [logs[slot, g][:, h * span : (h + 1) * span] for slot in range(pairs)]
            for part in range(pairs):
                line = lines[0]
                for slot in range(1, pairs):
                    line = jnp.where(part_of(slot) == part, lines[slot], line)
                log_ref[g * share + h : g * share + h + 1, part * span : (part + 1) * span] = line

    loads[6].wait()
    wait_here(wo.at[0, 1 - core], wo_recv.at[0])

    model = wo.shape[3]
    step_cols = 512
    wait_here(att_in.at[0, 1 - core], att_recv.at[0])
    for n in range(model // step_cols):
        at = slice(n * step_cols, (n + 1) * step_cols)
        res[:, at] = jnp.dot(att_in[0, 0], wo[0, 0, :, at], preferred_element_type=F32) + jnp.dot(
            att_in[0, 1], wo[0, 1, :, at], preferred_element_type=F32
        )
    swap_second(1, 1)
    ring_third(1)
    swap_second(0, 1)
    for unit in [0] + late_units:
        sent_kv(unit)
    tokens_sent()
    for slot in range(1, pairs):
        wait_here(att_in.at[slot], att_recv.at[slot])
    for slot in range(1, pairs):
        for n in range(model // step_cols):
            at = slice(n * step_cols, (n + 1) * step_cols)
            res[:, at] += jnp.dot(att_in[slot, core], wo[slot, core, :, at], preferred_element_type=F32)
    wo_last()
    for n in range(model // step_cols):
        at = slice(n * step_cols, (n + 1) * step_cols)
        total = res[:, at]
        for slot in range(1, pairs):
            total = total + jnp.dot(att_in[slot, 1 - core], wo[slot, 1 - core, :, at], preferred_element_type=F32)
        mixed_ref[:, at] = total.astype(BF16)

    wait_sent(att_out.at[0, 0], att_send.at[0])
    for slot in range(1, pairs):
        wait_sent(att_out.at[slot], att_send.at[slot])
    wo_sent()


def body(n_sp, n_tp, tokens, query_weight, key_weight, value_weight, out_weight, query_gain, key_gain):
    rows, depth = tokens.shape
    query_cols = query_weight.shape[1]
    kv_cols = key_weight.shape[1]
    heads, width = query_gain.shape
    kv_heads = key_gain.shape[0]
    group, model = out_weight.shape
    count = rows * n_tp
    pairs, cols = n_tp // 2, n_sp // 2
    sizes = (rows // 2, rows - rows // 2)
    chunks = len(sizes)
    span = 2 * rows
    units = 1 + (pairs - 1) * chunks
    spots = pairs * heads * span // TILE
    any_space = pl.BlockSpec(memory_space=pl.ANY)
    vmem = pl.BlockSpec(memory_space=pltpu.VMEM)
    dma = pltpu.SemaphoreType.DMA
    return pl.pallas_call(
        functools.partial(kernel, n_sp, n_tp, sizes),
        out_shape=(
            pltpu.VMEM((rows, model), BF16),
            pltpu.VMEM((heads, count), F32),
        ),
        in_specs=[any_space] * 7,
        out_specs=(vmem, vmem),
        scratch_shapes=[
            pltpu.VMEM((pairs, 2, rows, depth), BF16),
            pltpu.VMEM((depth, query_cols + 2 * kv_cols), BF16),
            pltpu.VMEM((2 * kv_cols, depth), BF16),
            pltpu.VMEM((pairs, 2, group, model), BF16),
            pltpu.VMEM((heads, width), BF16),
            pltpu.VMEM((kv_heads, width), BF16),
            pltpu.VMEM((128, 128), F32),
            pltpu.VMEM((pairs, span, query_cols), F32),
            pltpu.VMEM((pairs, 4, width // 4, span), F32),
            [pltpu.VMEM((4, width // 4, 2 * size), F32) for size in sizes] * (pairs - 1),
            pltpu.VMEM((pairs, kv_heads, width, heads // kv_heads * span), BF16),
            pltpu.VMEM((n_sp, span, 2 * kv_cols), BF16),
            [pltpu.VMEM((n_sp, 2 * size, 2 * kv_cols), BF16) for size in sizes] * (pairs - 1),
            pltpu.VMEM((spots, 1, TILE), F32),
            pltpu.VMEM((spots, width + ONES, TILE), F32),
            pltpu.VMEM((pairs, 2, rows, group), BF16),
            pltpu.VMEM((pairs, 2, rows, group), BF16),
            pltpu.VMEM((rows, model), F32),
            dma((5,)),
            dma((2 * pairs - 1,)),
            dma((1 + (pairs - 1) * 2 * chunks,)),
            dma((1 + (pairs - 1) * 3,)),
            dma((1 + (pairs - 1) * (ACROSS + 2 * ASIDE + 1),)),
            dma((units,)),
            dma((units, cols + 1)),
            dma((pairs,)),
            dma((pairs,)),
        ],
        compiler_params=pltpu.CompilerParams(
            collective_id=0, has_side_effects=True, vmem_limit_bytes=60 * 1024 * 1024
        ),
        name="attention",
    )(tokens, query_weight, key_weight.T, value_weight.T, out_weight, query_gain, key_gain)


def solution(mesh):
    return jax.shard_map(
        functools.partial(body, mesh.shape["sp"], mesh.shape["tp"]),
        mesh=mesh,
        in_specs=(
            P(("sp", "tp"), None),
            P(None, "tp"),
            P(None, "tp"),
            P(None, "tp"),
            P("tp", None),
            P("tp", None),
            P("tp", None),
        ),
        out_specs=(P(("sp", "tp"), None), P("tp", "sp")),
        check_vma=False,
    )
```

```python
import functools
import math

import jax
import jax.numpy as jnp
from jax import lax
from jax.experimental import pallas as pl
from jax.experimental.pallas import tpu as pltpu
from jax.sharding import PartitionSpec as P

GRID_W = 64
ROPE_BASE = 10000.0
EPS = 1e-06
LOG2E = math.log2(math.e)
LN2 = math.log(2.0)
ONES = 16
TILE = 256
AHEAD = 3
BEHIND = 3
LINES = 4
UNITS = 16
ACROSS = 6
ASIDE = 5
MESH = pl.DeviceIdType.MESH
F32 = jnp.float32
BF16 = jnp.bfloat16


def prepare(x, gain, tables):
    quarter = x.shape[0] // 4
    x = x * lax.rsqrt(jnp.mean(x * x, axis=0, keepdims=True) + EPS) * gain
    a, b, c, d = (x[i * quarter : (i + 1) * quarter] for i in range(4))
    row_cos, row_sin, col_cos, col_sin = tables
    return jnp.concatenate(
        [
            a * row_cos - b * row_sin,
            b * row_cos + a * row_sin,
            c * col_cos - d * col_sin,
            d * col_cos + c * col_sin,
        ],
        axis=0,
    )


def angle_tables(place, quarter):
    order = lax.broadcasted_iota(jnp.int32, (quarter, place.shape[1]), 0).astype(F32)
    freq = jnp.exp(order * (-math.log(ROPE_BASE) / quarter))
    shift = GRID_W.bit_length() - 1
    row = lax.shift_right_logical(place, shift).astype(F32) * freq
    col = jnp.bitwise_and(place, GRID_W - 1).astype(F32) * freq
    return (jnp.cos(row), jnp.sin(row), jnp.cos(col), jnp.sin(col))


def kernel(
    n_sp,
    n_tp,
    sizes,
    tok_hbm,
    wq_hbm,
    wk_hbm,
    wv_hbm,
    wo_hbm,
    qg_hbm,
    kg_hbm,
    mixed_ref,
    log_ref,
    tok,
    wall,
    wkv,
    wo,
    qg,
    kg,
    gains,
    raw,
    tabs,
    tabs_late,
    queries,
    kv_early,
    kv_late,
    top,
    acc,
    att_out,
    att_in,
    res,
    local_sem,
    tok_send,
    tok_recv,
    wo_send,
    wo_recv,
    kv_send,
    kv_recv,
    att_send,
    att_recv,
):
    sp = lax.axis_index("sp")
    tp = lax.axis_index("tp")
    pairs = n_tp // 2
    cols = n_sp // 2
    pair, core = tp // 2, tp % 2
    mate = pair * 2 + (1 - core)
    col, side = sp // 2, sp % 2
    other = col * 2 + (1 - side)

    def near_place(k):
        place, bit = col, 1
        while bit < cols:
            if k & bit:
                place = place + bit * (1 - 2 * ((col // bit) % 2))
            bit *= 2
        return place

    beside = near_place(1) * 2 + side
    rows = tok.shape[2]
    heads, width = qg.shape
    kv_heads = kg.shape[0]
    share = heads // kv_heads
    span = 2 * rows
    count = rows * n_tp
    query_cols = wq_hbm.shape[1]
    kv_cols = wk_hbm.shape[0]
    group = wo.shape[2]
    chunks = len(sizes)
    starts = [sum(sizes[:c]) for c in range(chunks)]
    quarter = width // 4

    def across(i):
        return lax.rem(pair + i, pairs) * 2 + core

    loads = [
        pltpu.make_async_copy(src, dst, local_sem.at[i])
        for i, src, dst in (
            (0, tok_hbm, tok.at[0, core]),
            (1, wk_hbm, wkv.at[0:kv_cols]),
            (1, wv_hbm, wkv.at[kv_cols:]),
            (1, wq_hbm, wall.at[:, 0:query_cols]),
            (2, qg_hbm, qg),
            (3, kg_hbm, kg),
            (4, wo_hbm, wo.at[0, core]),
        )
    ]
    for load in loads:
        load.start()

    barrier = pltpu.get_barrier_semaphore()
    peers = 0
    for i in range(1, n_tp):
        pl.semaphore_signal(barrier, inc=1, device_id={"tp": lax.rem(tp + i, n_tp)}, device_id_type=MESH)
        peers += 1
    pl.semaphore_signal(barrier, inc=1, device_id={"sp": other}, device_id_type=MESH)
    peers += 1
    for i in range(1, cols):
        peer = lax.rem(col + i, cols) * 2 + side
        pl.semaphore_signal(barrier, inc=1, device_id={"sp": peer}, device_id_type=MESH)
        peers += 1
    pl.semaphore_wait(barrier, peers)

    def send(src, dst, send_sem, recv_sem, where):
        return pltpu.make_async_remote_copy(
            src_ref=src,
            dst_ref=dst,
            send_sem=send_sem,
            recv_sem=recv_sem,
            device_id=where,
            device_id_type=MESH,
        )

    def wait_sent(spot, sem):
        send(spot, spot, sem, tok_recv.at[0], {"tp": mate}).wait_send()

    def wait_here(spot, sem):
        send(spot, spot, tok_send.at[0], sem, {"tp": mate}).wait_recv()

    def rows_of(c):
        return slice(starts[c], starts[c] + sizes[c])

    def tok_sem(which, slot, c):
        return tok_recv.at[1 + ((slot - 1) * 2 + which) * chunks + c]

    def token_over(i, c):
        slot = pairs - i
        return send(
            tok.at[0, core, rows_of(c)],
            tok.at[slot, core, rows_of(c)],
            tok_send.at[2 * i - 1],
            tok_sem(0, slot, c),
            {"tp": across(i)},
        )

    def token_on(slot, c):
        spot = tok.at[slot, core, rows_of(c)]
        return send(spot, spot, tok_send.at[2 * slot], tok_sem(1, slot, c), {"tp": mate})

    loads[0].wait()
    for c in range(chunks):
        for i in range(1, pairs):
            token_over(i, c).start()
    send(tok.at[0, core], tok.at[0, core], tok_send.at[0], tok_recv.at[0], {"tp": mate}).start()

    def tokens_sent():
        for n in range(2 * pairs - 1):
            wait_sent(tok.at[0, 0], tok_send.at[n])

    unit_rows = group // UNITS
    color = sp % 4
    colors = (color + 1 - 2 * (color % 2), (color + 2) % 4)
    color_far = 3 - color
    sides = (side, col % 2)
    friends = (other, beside)

    def ring_unit(whose, h):
        return whose * 2 + h

    def swap_unit(way, whose, h):
        return 8 + way * 4 + whose * 2 + h

    def wo_at(ref, unit):
        return ref.at[pl.ds(pl.multiple_of(unit * unit_rows, unit_rows), unit_rows)]

    def arrival(slot, number):
        return 1 + (slot - 1) * (ACROSS + 2 * ASIDE + 1) + number

    over = [(ring_unit(color, h), h) for h in range(2)]
    over += [(swap_unit(way, sides[way], h), 2 + way * 2 + h) for h in range(2) for way in (1, 0)]

    def wo_over(i, unit, number):
        slot = pairs - i
        return send(
            wo_at(wo_hbm, unit), wo_at(wo.at[slot, core], unit), wo_send.at[3 * i - 2 + 0], wo_recv.at[arrival(slot, number)], {"tp": across(i)}
        )

    def wo_aside(slot, unit, way, number):
        spot = wo_at(wo.at[slot, core], unit)
        return send(spot, spot, wo_send.at[3 * slot - 2 + 1], wo_recv.at[arrival(slot, ACROSS + way * ASIDE + number)], {"sp": friends[way]})

    def wo_got(slot, unit, number):
        spot = wo_at(wo.at[slot, core], unit)
        wait_here(spot, wo_recv.at[arrival(slot, number)])
        send(spot, spot, wo_send.at[3 * slot - 2 + 2], wo_recv.at[arrival(slot, ACROSS + 2 * ASIDE)], {"tp": mate}).start()

    send(wo_hbm, wo.at[0, core], wo_send.at[0], wo_recv.at[0], {"tp": mate}).start()
    for unit, number in over:
        for i in range(1, pairs):
            wo_over(i, unit, number).start()

    def ring_first(h):
        for slot in range(1, pairs):
            wo_got(slot, ring_unit(color, h), h)
            for way in range(2):
                wo_aside(slot, ring_unit(color, h), way, h).start()

    def ring_second(h):
        for slot in range(1, pairs):
            for way in range(2):
                wo_got(slot, ring_unit(colors[way], h), ACROSS + way * ASIDE + h)
                if way != h:
                    wo_aside(slot, ring_unit(colors[way], h), 1 - way, 4).start()

    def ring_third(h):
        for slot in range(1, pairs):
            wo_got(slot, ring_unit(color_far, h), ACROSS + h * ASIDE + 4)

    def swap_first(way, h):
        for slot in range(1, pairs):
            wo_got(slot, swap_unit(way, sides[way], h), 2 + way * 2 + h)
            wo_aside(slot, swap_unit(way, sides[way], h), way, 2 + h).start()

    def swap_second(way, h):
        for slot in range(1, pairs):
            wo_got(slot, swap_unit(way, 1 - sides[way], h), ACROSS + way * ASIDE + 2 + h)

    def wo_last():
        for slot in range(1, pairs):
            wait_here(wo.at[slot, 1 - core], wo_recv.at[arrival(slot, ACROSS + 2 * ASIDE)])

    def wo_sent():
        wait_sent(wo.at[0, 0], wo_send.at[0])
        for slot in range(1, pairs):
            wait_sent(wo.at[0, 0, 0 : ACROSS * unit_rows], wo_send.at[3 * slot - 2 + 0])
            wait_sent(wo.at[0, 0, 0 : 2 * ASIDE * unit_rows], wo_send.at[3 * slot - 2 + 1])
            wait_sent(wo.at[0, 0], wo_send.at[3 * slot - 2 + 2])

    def part_of(slot):
        return lax.rem(pair + slot, pairs)

    for slot in range(pairs):
        lane = lax.broadcasted_iota(jnp.int32, (quarter, span), 1)
        first = sp * count + part_of(slot) * span
        for n, table in enumerate(angle_tables(first + lane, quarter)):
            tabs[slot, n] = table
    for slot in range(1, pairs):
        for c in range(chunks):
            lane = lax.broadcasted_iota(jnp.int32, (quarter, 2 * sizes[c]), 1)
            lane = jnp.where(lane < sizes[c], lane, lane + (rows - sizes[c]))
            first = sp * count + part_of(slot) * span + starts[c]
            for n, table in enumerate(angle_tables(first + lane, quarter)):
                tabs_late[(slot - 1) * chunks + c][n] = table
    top[...] = jnp.full_like(top, -1e30)
    acc[...] = jnp.zeros_like(acc)
    pltpu.make_async_copy(wall, wall, local_sem.at[1]).wait()
    for load in loads[4:6]:
        load.wait()
    wall[:, query_cols:] = jnp.transpose(wkv[...])
    gains[...] = jnp.zeros_like(gains)
    gains[0:heads, 0:width] = qg[...].astype(F32) * (LOG2E * width ** (-0.5))
    gains[heads : heads + kv_heads, 0:width] = kg[...].astype(F32)
    turned_gains = jnp.transpose(gains[...])
    kv_rows = kv_heads * width

    def make_kv(x, tables, put):
        turned = jnp.transpose(x[:, 0:kv_rows])
        for g in range(kv_heads):
            gain = turned_gains[0:width, heads + g : heads + g + 1]
            keys = prepare(turned[g * width : (g + 1) * width], gain, tables)
            put(slice(g * width, (g + 1) * width), jnp.transpose(keys).astype(BF16))
        put(slice(kv_rows, 2 * kv_rows), x[:, kv_rows:].astype(BF16))

    def make_queries(slot):
        turned = jnp.transpose(raw[slot])
        tables = tuple(tabs[slot, n] for n in range(4))
        for g in range(kv_heads):
            made = []
            for h in range(g * share, (g + 1) * share):
                q = prepare(turned[h * width : (h + 1) * width], turned_gains[0:width, h : h + 1], tables)
                made.append(q.astype(BF16))
            queries[slot, g] = jnp.concatenate(made, axis=1)

    def kv_ref(unit):
        return kv_early if unit == 0 else kv_late[unit - 1]

    def kv_copy(unit, block, number, where):
        spot = kv_ref(unit).at[block]
        return send(spot, spot, kv_send.at[unit], kv_recv.at[unit, number], {"sp": where})

    def send_kv(unit):
        kv_copy(unit, sp, 0 if unit else cols, other).start()
        for k in range(1, cols):
            kv_copy(unit, sp, k, near_place(k) * 2 + side).start()

    def forward_kv(unit, start, stop):
        for k in range(start, stop):
            block = near_place(k) * 2 + side
            kv_copy(unit, block, k, other).wait_recv()
            kv_copy(unit, block, 0, other).start()

    def mirrored_kv(unit):
        if unit == 0:
            wait_here(kv_early.at[0 : cols - 1], kv_recv.at[0, 0])
        else:
            wait_here(kv_ref(unit).at[0:cols], kv_recv.at[unit, 0])

    def sent_kv(unit):
        wait_sent(kv_ref(unit).at[0 : n_sp - 1], kv_send.at[unit])

    wait_here(tok.at[0, 1 - core], tok_recv.at[0])
    depth = tok.shape[3]
    x = jnp.dot(tok[0].reshape(span, depth), wall[:, query_cols:], preferred_element_type=F32)

    def put_early(at, value):
        kv_early[sp, :, at] = value

    make_kv(x, tuple(tabs[0, n] for n in range(4)), put_early)
    send_kv(0)
    raw[0] = jnp.dot(tok[0].reshape(span, depth), wall[:, 0:query_cols], preferred_element_type=F32)
    make_queries(0)

    tiles = share * span // TILE

    def attend(loaders, slots):
        items = [(n, slot, g, t) for n in range(len(loaders)) for slot in slots for g in range(kv_heads) for t in range(tiles)]
        held = {}
        for n, load in enumerate(loaders):
            block = load()
            turned = jnp.transpose(block)
            ones = jnp.ones((ONES, block.shape[0]), BF16)
            for g in range(kv_heads):
                keys = block[:, g * width : (g + 1) * width]
                values = turned[kv_rows + g * width : kv_rows + (g + 1) * width]
                held[n, g] = (keys, jnp.concatenate([values, ones], axis=0))
        scores, weights = {}, {}

        def spot(i):
            _, slot, g, t = items[i]
            return (slot * kv_heads + g) * tiles + t

        def score(i):
            n, slot, g, t = items[i]
            q = queries[slot, g, :, t * TILE : (t + 1) * TILE]
            scores[i] = jnp.dot(held[n, g][0], q, preferred_element_type=F32)

        def soften(i):
            s = scores.pop(i)
            at = spot(i)
            old = top[at]
            new = jnp.maximum(old, jnp.max(s, axis=0, keepdims=True))
            top[at] = new
            weights[i] = (jnp.exp2(s - new).astype(BF16), jnp.exp2(old - new))

        def gather(i):
            n, slot, g, t = items[i]
            w, scale = weights.pop(i)
            at = spot(i)
            acc[at] = acc[at] * scale + jnp.dot(held[n, g][1], w, preferred_element_type=F32)

        total = len(items)
        for i in range(min(AHEAD, total)):
            score(i)
        for i in range(total):
            if i + AHEAD < total:
                score(i + AHEAD)
            if i >= BEHIND:
                gather(i - BEHIND)
            soften(i)
        for i in range(max(total - BEHIND, 0), total):
            gather(i)

    def early_blocks(*blocks):
        def load():
            return jnp.concatenate([kv_early[near_place(k) * 2 + way] for k, way in blocks], axis=0)

        return load

    def late_line(unit, k, way):
        def load():
            return jnp.concatenate([kv_late[unit - 1][(k + n) * 2 + way] for n in range(LINES)], axis=0)

        return load

    late_units = [1 + (slot - 1) * chunks + c for slot in range(1, pairs) for c in range(chunks)]
    late_order = [(slot, c) for c in range(chunks) for slot in range(1, pairs)]

    def token_first(slot, c):
        wait_here(tok.at[slot, core, rows_of(c)], tok_sem(0, slot, c))
        token_on(slot, c).start()

    def token_second(slot, c):
        unit = 1 + (slot - 1) * chunks + c
        wait_here(tok.at[slot, 1 - core, rows_of(c)], tok_sem(1, slot, c))
        piece = tok[slot, :, rows_of(c)].reshape(2 * sizes[c], depth)
        x = jnp.dot(piece, wall[:, query_cols:], preferred_element_type=F32)

        def put_late(at, value):
            kv_late[unit - 1][sp, :, at] = value

        make_kv(x, tuple(tabs_late[unit - 1][n] for n in range(4)), put_late)
        send_kv(unit)
        x = jnp.dot(piece, wall[:, 0:query_cols], preferred_element_type=F32)
        for which in range(2):
            at = slice(which * rows + starts[c], which * rows + starts[c] + sizes[c])
            raw[slot, at] = x[which * sizes[c] : (which + 1) * sizes[c]]

    def attend_early(slots, ways):
        for k in range(0, cols, LINES):
            attend([early_blocks((k + n, way), (k + n + 1, way)) for way in ways for n in range(0, LINES, 2)], slots)

    def attend_late(units, ways, slots):
        for k in range(0, cols, LINES):
            attend([late_line(unit, k, way) for unit in units for way in ways], slots)

    remote = list(range(1, pairs))
    everyone = remote + [0]
    firsts, last = late_units[:-1], late_units[-1]
    wait_here(kv_early.at[0], kv_recv.at[0, cols])
    attend([early_blocks((0, side), (0, 1 - side))], [0])
    forward_kv(0, 1, 3)
    for slot, c in late_order[:1]:
        token_first(slot, c)
    forward_kv(0, 3, cols)
    for slot, c in late_order[:1]:
        token_second(slot, c)
    for slot, c in late_order[1:-1]:
        token_first(slot, c)
        token_second(slot, c)
    attend([early_blocks(*((n, side) for n in range(1, LINES)))], [0])
    for slot, c in late_order[-1:]:
        token_first(slot, c)
    for unit in firsts:
        forward_kv(unit, 1, 2)
    for slot, c in late_order[-1:]:
        token_second(slot, c)
    for unit in firsts:
        forward_kv(unit, 2, cols)
    ring_first(0)
    for slot in remote:
        make_queries(slot)
    mirrored_kv(0)
    attend([early_blocks(*((n, 1 - side) for n in range(1, LINES)))], [0])
    for k in range(LINES, cols, LINES):
        attend([early_blocks((k + n, way), (k + n + 1, way)) for way in (side, 1 - side) for n in range(0, LINES, 2)], [0])
    forward_kv(last, 1, 2)
    ring_first(1)
    swap_first(1, 0)
    attend_early(remote, [side])
    forward_kv(last, 2, cols)
    attend_early(remote, [1 - side])
    swap_first(0, 0)
    for unit in firsts:
        mirrored_kv(unit)
    attend_late(firsts, [side, 1 - side], remote)
    swap_first(1, 1)
    ring_second(0)
    attend_late(firsts, [side, 1 - side], [0])
    swap_first(0, 1)
    ring_second(1)
    swap_second(1, 0)
    mirrored_kv(last)
    attend_late([last], [side, 1 - side], remote)

    logs = {}

    def att_copy(slot, which):
        there = 0 if slot == 0 else pairs - slot
        return send(
            att_out.at[slot, which],
            att_in.at[there, core],
            att_send.at[slot],
            att_recv.at[there],
            {"tp": part_of(slot) * 2 + which},
        )

    def finish(slot):
        turned = []
        for g in range(kv_heads):
            made, sums = [], []
            for t in range(tiles):
                at = (slot * kv_heads + g) * tiles + t
                total = acc[at, width : width + 1, :]
                made.append((acc[at, 0:width, :] * (1.0 / total)).astype(BF16))
                sums.append((top[at] + jnp.log2(total)) * LN2)
            turned.append(jnp.transpose(jnp.concatenate(made, axis=1)))
            logs[slot, g] = jnp.concatenate(sums, axis=1)
        for which in range(2):
            piece = jnp.concatenate(
                [
                    turned[g][h * span + which * rows : h * span + (which + 1) * rows]
                    for g in range(kv_heads)
                    for h in range(share)
                ],
                axis=1,
            )
            if slot:
                att_out[slot, which] = piece
                att_copy(slot, which).start()
            else:

                @pl.when(core == which)
                def _():
                    att_in[0, which] = piece

                @pl.when(core != which)
                def _():
                    att_out[0, which] = piece

    for slot in remote:
        finish(slot)
    attend_late([last], [side, 1 - side], [0])
    finish(0)
    att_copy(0, 1 - core).start()
    swap_second(0, 0)
    ring_third(0)
    for g in range(kv_heads):
        for h in range(share):
            lines = [logs[slot, g][:, h * span : (h + 1) * span] for slot in range(pairs)]
            for part in range(pairs):
                line = lines[0]
                for slot in range(1, pairs):
                    line = jnp.where(part_of(slot) == part, lines[slot], line)
                log_ref[g * share + h : g * share + h + 1, part * span : (part + 1) * span] = line

    loads[6].wait()
    wait_here(wo.at[0, 1 - core], wo_recv.at[0])

    model = wo.shape[3]
    step_cols = 512
    wait_here(att_in.at[0, 1 - core], att_recv.at[0])
    for n in range(model // step_cols):
        at = slice(n * step_cols, (n + 1) * step_cols)
        res[:, at] = jnp.dot(att_in[0, 0], wo[0, 0, :, at], preferred_element_type=F32) + jnp.dot(
            att_in[0, 1], wo[0, 1, :, at], preferred_element_type=F32
        )
    swap_second(1, 1)
    ring_third(1)
    swap_second(0, 1)
    for unit in [0] + late_units:
        sent_kv(unit)
    tokens_sent()
    for slot in range(1, pairs):
        wait_here(att_in.at[slot], att_recv.at[slot])
    for slot in range(1, pairs):
        for n in range(model // step_cols):
            at = slice(n * step_cols, (n + 1) * step_cols)
            res[:, at] += jnp.dot(att_in[slot, core], wo[slot, core, :, at], preferred_element_type=F32)
    wo_last()
    for n in range(model // step_cols):
        at = slice(n * step_cols, (n + 1) * step_cols)
        total = res[:, at]
        for slot in range(1, pairs):
            total = total + jnp.dot(att_in[slot, 1 - core], wo[slot, 1 - core, :, at], preferred_element_type=F32)
        mixed_ref[:, at] = total.astype(BF16)

    wait_sent(att_out.at[0, 0], att_send.at[0])
    for slot in range(1, pairs):
        wait_sent(att_out.at[slot], att_send.at[slot])
    wo_sent()


def body(n_sp, n_tp, tokens, query_weight, key_weight, value_weight, out_weight, query_gain, key_gain):
    rows, depth = tokens.shape
    query_cols = query_weight.shape[1]
    kv_cols = key_weight.shape[1]
    heads, width = query_gain.shape
    kv_heads = key_gain.shape[0]
    group, model = out_weight.shape
    count = rows * n_tp
    pairs, cols = n_tp // 2, n_sp // 2
    sizes = (rows // 2, rows - rows // 2)
    chunks = len(sizes)
    span = 2 * rows
    units = 1 + (pairs - 1) * chunks
    spots = pairs * heads * span // TILE
    any_space = pl.BlockSpec(memory_space=pl.ANY)
    vmem = pl.BlockSpec(memory_space=pltpu.VMEM)
    dma = pltpu.SemaphoreType.DMA
    return pl.pallas_call(
        functools.partial(kernel, n_sp, n_tp, sizes),
        out_shape=(
            pltpu.VMEM((rows, model), BF16),
            pltpu.VMEM((heads, count), F32),
        ),
        in_specs=[any_space] * 7,
        out_specs=(vmem, vmem),
        scratch_shapes=[
            pltpu.VMEM((pairs, 2, rows, depth), BF16),
            pltpu.VMEM((depth, query_cols + 2 * kv_cols), BF16),
            pltpu.VMEM((2 * kv_cols, depth), BF16),
            pltpu.VMEM((pairs, 2, group, model), BF16),
            pltpu.VMEM((heads, width), BF16),
            pltpu.VMEM((kv_heads, width), BF16),
            pltpu.VMEM((128, 128), F32),
            pltpu.VMEM((pairs, span, query_cols), F32),
            pltpu.VMEM((pairs, 4, width // 4, span), F32),
            [pltpu.VMEM((4, width // 4, 2 * size), F32) for size in sizes] * (pairs - 1),
            pltpu.VMEM((pairs, kv_heads, width, heads // kv_heads * span), BF16),
            pltpu.VMEM((n_sp, span, 2 * kv_cols), BF16),
            [pltpu.VMEM((n_sp, 2 * size, 2 * kv_cols), BF16) for size in sizes] * (pairs - 1),
            pltpu.VMEM((spots, 1, TILE), F32),
            pltpu.VMEM((spots, width + ONES, TILE), F32),
            pltpu.VMEM((pairs, 2, rows, group), BF16),
            pltpu.VMEM((pairs, 2, rows, group), BF16),
            pltpu.VMEM((rows, model), F32),
            dma((5,)),
            dma((2 * pairs - 1,)),
            dma((1 + (pairs - 1) * 2 * chunks,)),
            dma((1 + (pairs - 1) * 3,)),
            dma((1 + (pairs - 1) * (ACROSS + 2 * ASIDE + 1),)),
            dma((units,)),
            dma((units, cols + 1)),
            dma((pairs,)),
            dma((pairs,)),
        ],
        compiler_params=pltpu.CompilerParams(
            collective_id=0, has_side_effects=True, vmem_limit_bytes=60 * 1024 * 1024
        ),
        name="attention",
    )(tokens, query_weight, key_weight.T, value_weight.T, out_weight, query_gain, key_gain)


def solution(mesh):
    return jax.shard_map(
        functools.partial(body, mesh.shape["sp"], mesh.shape["tp"]),
        mesh=mesh,
        in_specs=(
            P(("sp", "tp"), None),
            P(None, "tp"),
            P(None, "tp"),
            P(None, "tp"),
            P("tp", None),
            P("tp", None),
            P("tp", None),
        ),
        out_specs=(P(("sp", "tp"), None), P("tp", "sp")),
        check_vma=False,
    )
```
